32 devices in a mesh: sp: 8 (over z, x), tp: 4 (over y, core).
Axes of the slice: x: 2, y: 2, z: 4, core: 2. Of those that a mesh axis runs over, the one named last changes fastest.
Arguments:
- skip_stream_input: bfloat16 [1024, 2048], P('sp'), may hold values from -16 to 16
- asking_vectors_split: bfloat16 [1024, 2048], P('sp', 'tp'), may hold values from -8 to 8
- lookup_vectors_split: bfloat16 [1024, 512], P('sp'), may hold values from -8 to 8
- content_vectors_split: bfloat16 [1024, 512], P('sp'), may hold values from -6 to 6
- asking_rms_gain: float32 [128], replicated, may hold values from 0.1 to 1.9
- lookup_rms_gain: float32 [128], replicated, may hold values from 0.1 to 1.9
- softness_per_channel: float32 [16], P('tp'), may hold values from 1.5 to 24
- mixing_exit_weights: bfloat16 [2048, 2048], P('tp'), may hold values from -0.125 to 0.125
- specialist_rms_gain: float32 [2048], replicated, may hold values from 0.1 to 1.9
- selected_dispatch_weights: float32 [1024, 2], P('sp'), may hold values from -6 to 6
- selected_specialist_ids: int32 [1024, 2], P('sp'), may hold values from 0 to 7, all different within a row; in each aligned block of 128 rows (0 to 127, 128 to 255, ...) at most 48 rows name the same one
- specialist_switch_weights: bfloat16 [8, 2048, 2048], P('sp', None, 'tp'), may hold values from -0.125 to 0.125
- specialist_widen_weights: bfloat16 [8, 2048, 2048], P('sp', None, 'tp'), may hold values from -0.125 to 0.125
- specialist_shrink_weights: bfloat16 [8, 2048, 2048], P('sp', 'tp'), may hold values from -0.125 to 0.125
Outputs:
- layer_out: bfloat16 [1024, 2048], P('sp', 'tp')
The draws below stay inside these ranges and needn't reach their ends.
Inputs may be any that keep to these rules, and one draw needn't show every extreme that they name: `selected_specialist_ids`: each row names 2 different experts. In each aligned block of 128 rows no expert is named by more than 48 rows, a bound that some block reaches.
All inputs are finite; a program needn't handle non-finite values.
Results may differ from the reference program's by a relative error of at most 0.0085.
Values may be sent and summed in bfloat16 or wider, within the bound.
A program may use at most 64 MiB of HBM per device.

```python
import math
import jax
import jax.numpy as jnp
import numpy as np
from jax import lax

D = 2048
CHANNEL_WIDTH = 128
HQ = 16
KVH = 4
GROUP = 4
EFF = 2048
TOP = 2
GRID_W = 64
TOK_DEV = 128
TOKENS = 1024
EXPERTS = 8
CAP = 48
HEADS_DEV = 4
EFF_DEV = 512
N_SP = 8
N_TP = 4


def query_key_pair(key):
    base_key = jax.random.fold_in(key, 71)
    key_one, key_two = jax.random.split(base_key, 2)
    key_draw = jax.random.normal(key_one, (TOKENS, KVH, CHANNEL_WIDTH), jnp.float32)
    query_draw = jax.random.normal(key_two, (TOKENS, HQ, CHANNEL_WIDTH), jnp.float32)
    query_out = jnp.clip(query_draw, -8.0, 8.0).reshape(TOKENS, HQ * CHANNEL_WIDTH)
    key_out = jnp.clip(key_draw, -8.0, 8.0).reshape(TOKENS, KVH * CHANNEL_WIDTH)
    return (query_out, key_out)


def draw_asking_vectors_split(key, part):
    return query_key_pair(key)[0].astype(jnp.bfloat16)


def draw_lookup_vectors_split(key, part):
    return query_key_pair(key)[1].astype(jnp.bfloat16)


def draw_softness_per_channel(key, part):
    own_key = jax.random.fold_in(key, 23)
    spread = jax.random.uniform(own_key, (HQ,), jnp.float32)
    return 1.5 * jnp.exp(spread * jnp.log(16.0 / 3.0))


def draw_skip_stream_input(key, part):
    own_key = jax.random.fold_in(key, 37)
    key_one, key_two, key_three = jax.random.split(own_key, 3)
    rising = jnp.exp(jnp.linspace(jnp.log(0.5), jnp.log(1.5), D))
    column_scale = rising * jnp.exp(jax.random.uniform(key_two, (D,), jnp.float32, jnp.log(0.6), jnp.log(1.7)))
    core = jax.random.normal(key_one, (TOKENS, D), jnp.float32)
    row_scale = jnp.exp(jax.random.uniform(key_three, (TOKENS, 1), jnp.float32, jnp.log(0.5), jnp.log(5.0)))
    drawn = core * row_scale * column_scale
    return jnp.clip(drawn, -16.0, 16.0).astype(jnp.bfloat16)


def block_levels(stream_key, dims, pieces, least, top_value):
    factor_of = 1.0
    for axis_at, blocks in pieces:
        heights = jax.random.uniform(jax.random.fold_in(jax.random.fold_in(stream_key, 6), axis_at), (blocks,), jnp.float32, least / len(pieces), top_value / len(pieces))
        factor_of = factor_of * jnp.repeat(jnp.exp(heights), dims[axis_at] // blocks).reshape((-1,) + (1,) * (len(dims) - 1 - axis_at))
    return factor_of


def routed_block(key, own, number, rows, count, top, reach, lean):
    order = jax.random.permutation(key, count)
    crowded, common = load_shares(count, rows * top, reach, lean, True), load_shares(count, rows * top, reach, lean, False)
    places = jnp.arange(count)

    def named(sizes, offset_by):
        used = int((sizes > 0).sum())
        fixed = max(1, used // 4)
        moved = fixed + (places - fixed + offset_by * (used - fixed)) % max(1, count - fixed)
        return jnp.zeros((count,), jnp.int32).at[order[jnp.where(places < fixed, places, moved)]].set(jnp.asarray(sizes, jnp.int32))

    sizes = jnp.where(number % 4 == 0, named(crowded, number // 4), named(common, number - number // 4 - 1))
    mixed = jax.random.permutation(jax.random.fold_in(own, 3), count)
    giver, receiver = mixed[0:count // 2 * 2:2], mixed[1:count // 2 * 2:2]
    slack = jnp.minimum(sizes[giver] - 1, reach - sizes[receiver]) // 2
    slack = jnp.where((giver == order[0]) | (receiver == order[0]) | (sizes[receiver] == 0), 0, jnp.maximum(slack, 0))
    moved = jax.random.randint(jax.random.fold_in(own, 4), (count // 2,), 0, 1 << 20) % (slack + 1)
    sizes = sizes.at[giver].add(-moved).at[receiver].add(moved)
    labels = jnp.searchsorted(jnp.cumsum(sizes), jnp.arange(rows * top), side="right").astype(jnp.int32)
    table = labels.reshape(top, rows).T
    table = table[jax.random.permutation(jax.random.fold_in(own, 1), rows)]
    offset_by = jax.random.randint(jax.random.fold_in(own, 2), (rows, 1), 0, top)
    return jnp.take_along_axis(table, (jnp.arange(top)[None, :] + offset_by) % top, axis=1)


def load_shares(number_of, total, most, slope, full):
    weights = [(1 << 20) // math.isqrt(grade ** slope) + 1 for grade in range(1, number_of + 1)]
    largest = most if full else min(most, max(-(-total // number_of), total * weights[0] // sum(weights)))
    least = 1 if total - largest >= number_of - 1 else 0
    given, spare = [largest] + [least] * (number_of - 1), total - largest - least * (number_of - 1)
    while spare > 0:
        candidates = [i for i in range(1, number_of) if given[i] < largest] or [i for i in range(1, number_of) if given[i] < most]
        whole, budget = sum([weights[i] for i in candidates]), spare
        for i in candidates:
            extra = min(most - given[i], max(1, budget * weights[i] // whole), spare)
            given[i] = given[i] + extra
            spare = spare - extra
    return np.array(given)


def centred(rng, extent, deviation, limit, cuts=(), held_as=jnp.bfloat16):
    values = jax.random.normal(rng, extent, jnp.float32) * deviation
    if len(cuts) > 0:
        values = block_levels(rng, extent, cuts, -0.22, 0.18) * values
    return jnp.clip(values, min=-limit, max=limit).astype(held_as)


def setup_inputs(seed: int = 0) -> dict:
    splits = jax.random.split(jax.random.key(seed), 15)
    skip_stream_input = draw_skip_stream_input(jax.random.fold_in(splits[14], 71), 0)
    asking_vectors_split = draw_asking_vectors_split(jax.random.fold_in(splits[14], 71), 0)
    lookup_vectors_split = draw_lookup_vectors_split(jax.random.fold_in(splits[14], 71), 0)
    content_vectors_split = centred(splits[3], (TOKENS, KVH * CHANNEL_WIDTH), 1.0, 6.0, ((0, 8),))
    asking_rms_gain = jnp.clip(1.0 + 0.18 * jax.random.normal(splits[4], (CHANNEL_WIDTH,), jnp.float32), 0.1, 1.9)
    lookup_rms_gain = jnp.clip(1.0 + 0.18 * jax.random.normal(splits[5], (CHANNEL_WIDTH,), jnp.float32), 0.1, 1.9)
    softness_per_channel = draw_softness_per_channel(jax.random.fold_in(splits[14], 71), 0)
    mixing_exit_weights = centred(splits[7], (HQ * CHANNEL_WIDTH, D), (HQ * CHANNEL_WIDTH) ** -0.5, 0.125, ((0, 4),))
    specialist_rms_gain = jnp.clip(1.0 + 0.18 * jax.random.normal(splits[8], (D,), jnp.float32), 0.1, 1.9)
    selected_dispatch_weights = centred(splits[9], (TOKENS, TOP), 1.5, 6.0, ((0, 8),), jnp.float32)
    selected_specialist_ids_keys = jax.random.split(jax.random.fold_in(splits[10], 1), TOKENS // TOK_DEV)
    selected_specialist_ids_turns = jax.random.permutation(jax.random.fold_in(splits[10], 3), TOKENS // TOK_DEV)
    selected_specialist_ids = jax.vmap(lambda own, number: routed_block(jax.random.fold_in(splits[10], 2), own, number, TOK_DEV, EXPERTS, TOP, CAP, 1))(selected_specialist_ids_keys, selected_specialist_ids_turns).reshape((TOKENS, TOP))
    specialist_switch_weights = centred(splits[11], (EXPERTS, D, EFF), D ** -0.5, 0.125, ((0, 8), (2, 4)))
    specialist_widen_weights = centred(splits[12], (EXPERTS, D, EFF), D ** -0.5, 0.125, ((0, 8), (2, 4)))
    specialist_shrink_weights = centred(splits[13], (EXPERTS, EFF, D), EFF ** -0.5, 0.125, ((0, 8), (1, 4)))
    return {"skip_stream_input": skip_stream_input, "asking_vectors_split": asking_vectors_split, "lookup_vectors_split": lookup_vectors_split, "content_vectors_split": content_vectors_split, "asking_rms_gain": asking_rms_gain, "lookup_rms_gain": lookup_rms_gain, "softness_per_channel": softness_per_channel, "mixing_exit_weights": mixing_exit_weights, "specialist_rms_gain": specialist_rms_gain, "selected_dispatch_weights": selected_dispatch_weights, "selected_specialist_ids": selected_specialist_ids, "specialist_switch_weights": specialist_switch_weights, "specialist_widen_weights": specialist_widen_weights, "specialist_shrink_weights": specialist_shrink_weights}


EPSILON = 1e-06

def kept(array_in):
    return lax.optimization_barrier(array_in)

def rotate_half(values_in, positions, full_width):
    half_width = full_width // 2
    frequency = 10000.0 ** (-jnp.arange(half_width, dtype=jnp.float32) / half_width)
    angles = positions.astype(jnp.float32)[:, None] * frequency[None, :]
    cosine = jnp.cos(angles)[:, None, :]
    sine = jnp.sin(angles)[:, None, :]
    leading = values_in[..., :half_width]
    trailing = values_in[..., half_width:]
    return jnp.concatenate([leading * cosine - trailing * sine, trailing * cosine + leading * sine], axis=-1)

def norm_rotate(heads_in, gain_vec, positions):
    widened = heads_in.astype(jnp.float32)
    scaled = widened * lax.rsqrt(lax.optimization_barrier(jnp.mean(widened * widened, axis=-1, keepdims=True)) + EPSILON) * gain_vec
    half_width = scaled.shape[-1] // 2
    grid_rows = positions // GRID_W
    grid_cols = positions % GRID_W
    turned = jnp.concatenate([rotate_half(scaled[..., :half_width], grid_rows, half_width), rotate_half(scaled[..., half_width:], grid_cols, half_width)], axis=-1)
    return kept(turned.astype(jnp.bfloat16))

def reference(skip_stream_input, asking_vectors_split, lookup_vectors_split, content_vectors_split, asking_rms_gain, lookup_rms_gain, softness_per_channel, mixing_exit_weights, specialist_rms_gain, selected_dispatch_weights, selected_specialist_ids, specialist_switch_weights, specialist_widen_weights, specialist_shrink_weights):
    positions = jnp.arange(TOKENS, dtype=jnp.int32)
    query_turned = norm_rotate(asking_vectors_split.reshape(TOKENS, HQ, CHANNEL_WIDTH), asking_rms_gain, positions)
    key_turned = norm_rotate(lookup_vectors_split.reshape(TOKENS, KVH, CHANNEL_WIDTH), lookup_rms_gain, positions)
    key_all = jnp.repeat(key_turned, GROUP, axis=1).astype(jnp.float32)
    value_all = jnp.repeat(content_vectors_split.reshape(TOKENS, KVH, CHANNEL_WIDTH), GROUP, axis=1).astype(jnp.float32)
    inverse_root_width = softness_per_channel / math.sqrt(CHANNEL_WIDTH)
    block_len = math.gcd(TOKENS, 512)
    query_blocks = query_turned.reshape(TOKENS // block_len, block_len, HQ, CHANNEL_WIDTH)

    def attend(query_block):
        scores = jnp.einsum('qhd,khd->hqk', query_block.astype(jnp.float32), key_all) * inverse_root_width[:, None, None]
        row_max = lax.optimization_barrier(jnp.max(scores, axis=-1, keepdims=True))
        exp_terms = jnp.exp(scores - row_max)
        denominator = lax.optimization_barrier(jnp.sum(exp_terms, axis=-1))
        probs = kept(exp_terms.astype(jnp.bfloat16)).astype(jnp.float32)
        weighted = jnp.einsum('hqk,khd->qhd', probs, value_all)
        return (weighted / jnp.transpose(denominator)[:, :, None]).astype(jnp.bfloat16)
    attention = kept(lax.map(attend, query_blocks).reshape(TOKENS, HQ * CHANNEL_WIDTH))
    group_width = HEADS_DEV * CHANNEL_WIDTH
    attended_sum = jnp.zeros((TOKENS, D), jnp.float32)
    for group_index in range(N_TP):
        lower = group_index * group_width
        part_sum = jnp.dot(attention[:, lower:lower + group_width], mixing_exit_weights[lower:lower + group_width], preferred_element_type=jnp.float32)
        attended_sum = attended_sum + kept(part_sum.astype(jnp.bfloat16)).astype(jnp.float32)
    attended = kept(attended_sum.astype(jnp.bfloat16))
    mid_rows = kept((skip_stream_input.astype(jnp.float32) + attended.astype(jnp.float32)).astype(jnp.bfloat16))
    mid_wide = mid_rows.astype(jnp.float32)
    normed = (mid_wide * lax.rsqrt(lax.optimization_barrier(jnp.mean(mid_wide * mid_wide, axis=-1, keepdims=True)) + EPSILON) * specialist_rms_gain).astype(jnp.bfloat16)
    route_weights = jax.nn.softmax(selected_dispatch_weights.astype(jnp.float32), axis=-1)
    flat_ids = selected_specialist_ids.reshape(N_SP, TOK_DEV * TOP).astype(jnp.int32)
    one_hot = (flat_ids[..., None] == jnp.arange(EXPERTS, dtype=jnp.int32)[None, None, :]).astype(jnp.int32)
    earlier = jnp.cumsum(one_hot, axis=1) - one_hot
    slot_index = lax.optimization_barrier(jnp.sum(earlier * one_hot, axis=-1)).astype(jnp.int32)
    block_ids = jnp.arange(N_SP, dtype=jnp.int32)[:, None]
    destination = (flat_ids * (N_SP * CAP) + block_ids * CAP + slot_index).reshape(-1).astype(jnp.int32)
    owner_rows = (jnp.arange(TOKENS * TOP, dtype=jnp.int32) // TOP).astype(jnp.int32)
    slot_owner = jnp.zeros((EXPERTS * N_SP * CAP,), jnp.int32).at[destination].set(owner_rows)
    filled = jnp.zeros((EXPERTS * N_SP * CAP,), jnp.int32).at[destination].set(1)
    routed = jnp.where(filled[:, None] > 0, normed[slot_owner], jnp.zeros((), jnp.bfloat16))
    routed = routed.reshape(EXPERTS, N_SP * CAP, D)

    def serve(operands):
        rows_in, gate_mat, up_mat, down_mat = operands
        gate_acc = jnp.dot(rows_in, gate_mat, preferred_element_type=jnp.float32)
        up_acc = jnp.dot(rows_in, up_mat, preferred_element_type=jnp.float32)
        hidden = kept((jax.nn.silu(gate_acc) * up_acc).astype(jnp.bfloat16))
        out_sum = jnp.zeros((rows_in.shape[0], D), jnp.float32)
        for group_index in range(N_TP):
            lower = group_index * EFF_DEV
            part_sum = jnp.dot(hidden[:, lower:lower + EFF_DEV], down_mat[lower:lower + EFF_DEV], preferred_element_type=jnp.float32)
            out_sum = out_sum + kept(part_sum.astype(jnp.bfloat16)).astype(jnp.float32)
        return out_sum.astype(jnp.bfloat16)
    expert_out = kept(lax.map(serve, (routed, specialist_switch_weights, specialist_widen_weights, specialist_shrink_weights)).reshape(-1, D))
    picked = expert_out[destination].reshape(TOKENS, TOP, D).astype(jnp.float32)
    layer_out = mid_wide + lax.optimization_barrier(jnp.sum(route_weights[..., None] * picked, axis=1))
    return layer_out.astype(jnp.bfloat16)
```

```python
import functools
import math

import jax
import jax.numpy as jnp
from jax import lax
from jax.experimental import pallas as pl
from jax.experimental.pallas import tpu as pltpu
from jax.sharding import PartitionSpec as P

CHANNEL_WIDTH = 128
GROUP = 4
GRID_W = 64
CORES = 2
EPSILON = 1e-06
MESH = pl.DeviceIdType.MESH
BF = jnp.bfloat16
F32 = jnp.float32


def turn_tables(positions):
    quarter = CHANNEL_WIDTH // 4
    frequency = 10000.0 ** (-jnp.arange(quarter, dtype=F32) / quarter)
    rows = (positions // GRID_W).astype(F32)[:, None] * frequency[None, :]
    cols = (positions % GRID_W).astype(F32)[:, None] * frequency[None, :]
    angles = jnp.concatenate([rows, rows, cols, cols], axis=1)
    cosine = jnp.cos(angles)
    sine = jnp.sin(angles)
    lane = jnp.arange(CHANNEL_WIDTH) // quarter
    first = (lane % 2 == 0)[None, :]
    return cosine, jnp.where(first, -sine, 0.0), jnp.where(first, 0.0, sine)


def norm_turn(x, gain, cosine, sine_a, sine_b):
    x = x.astype(F32)
    y = x * lax.rsqrt(jnp.mean(x * x, axis=-1, keepdims=True) + EPSILON) * gain
    quarter = CHANNEL_WIDTH // 4
    out = (
        y * cosine
        + pltpu.roll(y, CHANNEL_WIDTH - quarter, 1) * sine_a
        + pltpu.roll(y, quarter, 1) * sine_b
    )
    return out.astype(BF)


def dot(a, b):
    return jnp.dot(a, b, preferred_element_type=F32)


def layer_kernel(
    dims,
    skip_ref, q_ref, k_ref, v_ref, qg_ref, kg_ref, soft_ref, cos_ref, sa_ref, sb_ref,
    gain_ref, route_ref, ids_ref, wo_hbm, wg_hbm, wu_hbm, wd_hbm,
    out_ref,
    kk, vv, qs, sc, attn, pt, pk,
    p_send, p_recv, p_own, py_send, py_recv, mid,
    disp, xg, xn, r_send, r_recv, r_own, ry_send, ry_recv, ret, back,
    wo, wg, wu, wd,
    w_sem, k_s, k_r, v_s, v_r, pa_s, pa_r, py_s, py_r, d_s, d_r,
    gp_s, gp_r, gy_s, gy_r, gf_s, gf_r, rp_s, rp_r, ry_s, ry_r, b_s, b_r,
):
    n, m, tok, width, share, heads, lkv, capp, nch = dims
    A = m // CORES
    CW = CHANNEL_WIDTH
    me = lax.axis_index("sp")
    t = lax.axis_index("tp")
    a_pos = t // CORES
    core = t % CORES
    other = 1 - core
    partner = (me, a_pos * CORES + other)
    G = n // nch
    R = G * capp

    def sp_up(j):
        return (lax.rem(me + j, n), t)

    def sp_down(j):
        return (lax.rem(me + n - j, n), t)

    def a_at(i):
        return lax.rem(a_pos + i, A)

    def y_peer(i):
        return (me, a_at(i) * CORES + core)

    def cols_of(i, c):
        return pl.ds(pl.multiple_of((a_at(i) * CORES + c) * share, share), share)

    my_cols = pl.ds(pl.multiple_of(t * share, share), share)

    sends = []

    def remote(src, dst, ss, rs, dev):
        return pltpu.make_async_remote_copy(
            src_ref=src, dst_ref=dst, send_sem=ss, recv_sem=rs, device_id=dev, device_id_type=MESH
        )

    def go(cp):
        cp.start()
        sends.append(cp)
        return cp

    loads = [
        pltpu.make_async_copy(wo_hbm, wo, w_sem.at[0]),
        pltpu.make_async_copy(wg_hbm.at[0], wg, w_sem.at[1]),
        pltpu.make_async_copy(wu_hbm.at[0], wu, w_sem.at[2]),
        pltpu.make_async_copy(wd_hbm.at[0], wd, w_sem.at[3]),
    ]
    for cp in loads:
        cp.start()

    barrier = pltpu.get_barrier_semaphore()
    peers = [sp_up(j) for j in range(1, n)] + [partner] + [y_peer(i) for i in range(1, A)]
    for dev in peers:
        pl.semaphore_signal(barrier, inc=1, device_id=dev, device_id_type=MESH)

    first = (t * heads) // GROUP
    kv_cols = pl.ds(pl.multiple_of(first * CW, CW), lkv * CW)
    cosine, sine_a, sine_b = cos_ref[...], sa_ref[...], sb_ref[...]
    k_in = k_ref[:, kv_cols]
    for h in range(lkv):
        kk[0, :, h * CW:(h + 1) * CW] = norm_turn(
            k_in[:, h * CW:(h + 1) * CW], kg_ref[...], cosine, sine_a, sine_b
        )
    vv[0] = v_ref[:, kv_cols]
    pl.semaphore_wait(barrier, len(peers))
    k_cp, v_cp = {}, {}
    for j in range(1, n):
        k_cp[j] = go(remote(kk.at[0], kk.at[j], k_s.at[j], k_r.at[j], sp_up(j)))
    for j in range(1, n):
        v_cp[j] = go(remote(vv.at[0], vv.at[j], v_s.at[j], v_r.at[j], sp_up(j)))

    for h in range(heads):
        qs[h] = norm_turn(q_ref[:, h * CW:(h + 1) * CW], qg_ref[...], cosine, sine_a, sine_b)

    rel = ids_ref[...] - me
    rel = jnp.where(rel < 0, rel + n, rel)
    lanes = -(-n // 128) * 128
    lane_id = lax.broadcasted_iota(jnp.int32, (tok, lanes), 1)
    hot = [(rel[:, c:c + 1] == lane_id).astype(F32) for c in range(2)]
    lower = (
        lax.broadcasted_iota(jnp.int32, (tok, tok), 1)
        < lax.broadcasted_iota(jnp.int32, (tok, tok), 0)
    ).astype(F32)
    rank = dot(lower.astype(BF), (hot[0] + hot[1]).astype(BF))
    slot_id = lax.broadcasted_iota(jnp.int32, (tok, n * capp), 1).astype(F32)
    picks = []
    for c in range(2):
        place = rel[:, c:c + 1].astype(F32) * capp + jnp.sum(hot[c] * rank, axis=1, keepdims=True)
        picks.append((slot_id == place).astype(F32))
        pk[c] = picks[c].astype(BF)
    pt[...] = jnp.transpose(picks[0] + picks[1]).astype(BF)

    group = heads // lkv
    for j in range(n):
        if j:
            k_cp[j].wait_recv()
        for g in range(lkv):
            qg = qs[g * group:(g + 1) * group].reshape(group * tok, CW)
            s = lax.dot_general(
                qg, kk[j, :, g * CW:(g + 1) * CW], (((1,), (1,)), ((), ())),
                preferred_element_type=F32,
            )
            sc[pl.ds(g * group * tok, group * tok), j * tok:(j + 1) * tok] = s
    for j in range(1, n):
        v_cp[j].wait_recv()
    for h in range(heads):
        g = h // group
        s = sc[h * tok:(h + 1) * tok, :] * (soft_ref[h] * (1.0 / math.sqrt(CW)))
        e = jnp.exp(s - jnp.max(s, axis=-1, keepdims=True))
        total = jnp.sum(e, axis=-1, keepdims=True)
        v_all = vv[:, :, g * CW:(g + 1) * CW].reshape(n * tok, CW)
        attn[:, h * CW:(h + 1) * CW] = (dot(e.astype(BF), v_all) / total).astype(BF)

    loads[0].wait()
    att = attn[...]
    order = list(range(1, A)) + [0]
    pa_cp, py_cp = {}, {}
    for i in order:
        p_send[i] = dot(att, wo[:, cols_of(i, other)]).astype(BF)
        pa_cp[i] = go(remote(p_send.at[i], p_recv.at[i], pa_s.at[i], pa_r.at[i], partner))
    for i in order:
        p_own[i] = dot(att, wo[:, cols_of(i, core)])
    for i in range(1, A):
        pa_cp[i].wait_recv()
        py_send[i] = (p_own[i] + p_recv[i].astype(F32)).astype(BF)
        py_cp[i] = go(remote(py_send.at[i], py_recv.at[i], py_s.at[i], py_r.at[i], y_peer(i)))
    pa_cp[0].wait_recv()
    acc = p_own[0] + p_recv[0].astype(F32)
    for i in range(1, A):
        py_cp[i].wait_recv()
        acc = acc + py_recv[i].astype(F32)
    mid[...] = (skip_ref[:, my_cols].astype(F32) + acc.astype(BF).astype(F32)).astype(BF)

    disp[...] = dot(pt[...], mid[...]).astype(BF)
    d_cp = {}
    for j in range(1, n):
        d_cp[j] = go(remote(
            disp.at[pl.ds(j * capp, capp)], xg.at[pl.ds(j * capp, capp), my_cols],
            d_s.at[j], d_r.at[j], sp_up(j),
        ))
    xg[pl.ds(0, capp), my_cols] = disp[pl.ds(0, capp), :]

    gp_cp, gy_cp, gf_cp = {}, {}, {}
    for ch in range(nch):
        rows = pl.ds(ch * R, R)
        for j in range(ch * G, (ch + 1) * G):
            if j:
                d_cp[j].wait_recv()
        mine = xg.at[rows, my_cols]
        for i in range(1, A):
            gy_cp[ch, i] = go(remote(mine, mine, gy_s.at[ch, i], gy_r.at[ch, i], y_peer(i)))
        gp_cp[ch] = go(remote(mine, mine, gp_s.at[ch], gp_r.at[ch], partner))
    for ch in range(nch):
        rows = pl.ds(ch * R, R)
        for i in range(1, A):
            gy_cp[ch, i].wait_recv()
            piece = xg.at[rows, cols_of(A - i, core)]
            gf_cp[ch, i] = go(remote(piece, piece, gf_s.at[ch, i], gf_r.at[ch, i], partner))
    rp_cp, ry_cp = {}, {}
    for ch in range(nch):
        rows = pl.ds(ch * R, R)
        gp_cp[ch].wait_recv()
        for i in range(1, A):
            gf_cp[ch, i].wait_recv()
        x = xg[rows, :].astype(F32)
        xn[...] = (
            x * lax.rsqrt(jnp.mean(x * x, axis=-1, keepdims=True) + EPSILON) * gain_ref[...]
        ).astype(BF)
        if ch == 0:
            loads[1].wait()
            loads[2].wait()
        x = xn[...]
        gate = dot(x, wg[...])
        up = dot(x, wu[...])
        hidden = (gate / (1.0 + jnp.exp(-gate)) * up).astype(BF)
        if ch == 0:
            loads[3].wait()
        for i in order:
            r_send[ch, i] = dot(hidden, wd[:, cols_of(i, other)]).astype(BF)
            rp_cp[ch, i] = go(remote(
                r_send.at[ch, i], r_recv.at[ch, i], rp_s.at[ch, i], rp_r.at[ch, i], partner
            ))
        for i in order:
            r_own[ch, i] = dot(hidden, wd[:, cols_of(i, core)])
        for i in range(1, A):
            rp_cp[ch, i].wait_recv()
            ry_send[ch, i] = (r_own[ch, i] + r_recv[ch, i].astype(F32)).astype(BF)
            ry_cp[ch, i] = go(remote(
                ry_send.at[ch, i], ry_recv.at[ch, i], ry_s.at[ch, i], ry_r.at[ch, i], y_peer(i)
            ))
    b_cp = {}
    for ch in range(nch):
        rp_cp[ch, 0].wait_recv()
        acc = r_own[ch, 0] + r_recv[ch, 0].astype(F32)
        for i in range(1, A):
            ry_cp[ch, i].wait_recv()
            acc = acc + ry_recv[ch, i].astype(F32)
        ret[pl.ds(ch * R, R), :] = acc.astype(BF)
        for j in range(ch * G, (ch + 1) * G):
            rows = pl.ds(j * capp, capp)
            if j:
                b_cp[j] = go(remote(ret.at[rows], back.at[rows], b_s.at[j], b_r.at[j], sp_down(j)))
            else:
                back[rows, :] = ret[rows, :]

    route = route_ref[...]
    top = jnp.max(route, axis=1, keepdims=True)
    e = jnp.exp(route - top)
    weight = e / jnp.sum(e, axis=1, keepdims=True)
    for j in range(1, n):
        b_cp[j].wait_recv()
    got = back[...]
    out = weight[:, 0:1] * dot(pk[0], got) + weight[:, 1:2] * dot(pk[1], got)
    out_ref[...] = (mid[...].astype(F32) + out).astype(BF)
    for cp in sends:
        cp.wait_send()


def shards(
    skip, q, k, v, q_gain, k_gain, soft, mix, gain, route, ids, w_gate, w_up, w_down
):
    n, m = lax.axis_size("sp"), lax.axis_size("tp")
    tok, width = skip.shape
    share = width // m
    heads = q.shape[1] // CHANNEL_WIDTH
    lkv = max(1, heads // GROUP)
    cap = max(2, 3 * tok * ids.shape[1] // (2 * n))
    capp = -(-cap // 16) * 16
    nch = 2
    A = m // CORES
    eff = w_gate.shape[2]
    rows_all = n * capp
    R = rows_all // nch
    kvw = lkv * CHANNEL_WIDTH
    positions = lax.axis_index("sp") * tok + jnp.arange(tok, dtype=jnp.int32)
    cosine, sine_a, sine_b = turn_tables(positions)
    vm = pl.BlockSpec(memory_space=pltpu.VMEM)
    hbm = pl.BlockSpec(memory_space=pl.ANY)
    dma = pltpu.SemaphoreType.DMA
    dims = (n, m, tok, width, share, heads, lkv, capp, nch)
    pair = (nch, A)
    call = pl.pallas_call(
        functools.partial(layer_kernel, dims),
        out_shape=jax.ShapeDtypeStruct((tok, share), BF),
        in_specs=[vm] * 6 + [pl.BlockSpec(memory_space=pltpu.SMEM)] + [vm] * 6 + [hbm] * 4,
        out_specs=vm,
        scratch_shapes=[
            pltpu.VMEM((n, tok, kvw), BF),
            pltpu.VMEM((n, tok, kvw), BF),
            pltpu.VMEM((heads, tok, CHANNEL_WIDTH), BF),
            pltpu.VMEM((heads * tok, n * tok), F32),
            pltpu.VMEM((tok, heads * CHANNEL_WIDTH), BF),
            pltpu.VMEM((rows_all, tok), BF),
            pltpu.VMEM((2, tok, rows_all), BF),
            pltpu.VMEM((A, tok, share), BF),
            pltpu.VMEM((A, tok, share), BF),
            pltpu.VMEM((A, tok, share), F32),
            pltpu.VMEM((A, tok, share), BF),
            pltpu.VMEM((A, tok, share), BF),
            pltpu.VMEM((tok, share), BF),
            pltpu.VMEM((rows_all, share), BF),
            pltpu.VMEM((rows_all, width), BF),
            pltpu.VMEM((R, width), BF),
            pltpu.VMEM(pair + (R, share), BF),
            pltpu.VMEM(pair + (R, share), BF),
            pltpu.VMEM(pair + (R, share), F32),
            pltpu.VMEM(pair + (R, share), BF),
            pltpu.VMEM(pair + (R, share), BF),
            pltpu.VMEM((rows_all, share), BF),
            pltpu.VMEM((rows_all, share), BF),
            pltpu.VMEM(mix.shape, BF),
            pltpu.VMEM(w_gate.shape[1:], BF),
            pltpu.VMEM(w_up.shape[1:], BF),
            pltpu.VMEM(w_down.shape[1:], BF),
            dma((4,)),
            dma((n,)), dma((n,)), dma((n,)), dma((n,)),
            dma((A,)), dma((A,)), dma((A,)), dma((A,)),
            dma((n,)), dma((n,)),
            dma((nch,)), dma((nch,)), dma(pair), dma(pair), dma(pair), dma(pair),
            dma(pair), dma(pair), dma(pair), dma(pair),
            dma((n,)), dma((n,)),
        ],
        compiler_params=pltpu.CompilerParams(
            collective_id=0, has_side_effects=True, vmem_limit_bytes=56 * 1024 * 1024
        ),
    )
    return call(
        skip, q, k, v, q_gain.reshape(1, -1), k_gain.reshape(1, -1), soft,
        cosine, sine_a, sine_b, gain.reshape(1, -1), route, ids, mix, w_gate, w_up, w_down,
    )


def solution(mesh):
    in_specs = (
        P("sp", None),
        P("sp", "tp"),
        P("sp", None),
        P("sp", None),
        P(),
        P(),
        P("tp"),
        P("tp", None),
        P(),
        P("sp", None),
        P("sp", None),
        P("sp", None, "tp"),
        P("sp", None, "tp"),
        P("sp", "tp", None),
    )
    out_specs = P("sp", "tp")
    return jax.shard_map(shards, mesh=mesh, in_specs=in_specs, out_specs=out_specs, check_vma=False)
```

```python
import functools
import math

import jax
import jax.numpy as jnp
from jax import lax
from jax.experimental import pallas as pl
from jax.experimental.pallas import tpu as pltpu
from jax.sharding import PartitionSpec as P

CHANNEL_WIDTH = 128
GROUP = 4
GRID_W = 64
CORES = 2
EPSILON = 1e-06
MESH = pl.DeviceIdType.MESH
BF = jnp.bfloat16
F32 = jnp.float32


def turn_tables(positions):
    quarter = CHANNEL_WIDTH // 4
    frequency = 10000.0 ** (-jnp.arange(quarter, dtype=F32) / quarter)
    rows = (positions // GRID_W).astype(F32)[:, None] * frequency[None, :]
    cols = (positions % GRID_W).astype(F32)[:, None] * frequency[None, :]
    angles = jnp.concatenate([rows, rows, cols, cols], axis=1)
    cosine = jnp.cos(angles)
    sine = jnp.sin(angles)
    lane = jnp.arange(CHANNEL_WIDTH) // quarter
    first = (lane % 2 == 0)[None, :]
    return cosine, jnp.where(first, -sine, 0.0), jnp.where(first, 0.0, sine)


def norm_turn(x, gain, cosine, sine_a, sine_b):
    x = x.astype(F32)
    y = x * lax.rsqrt(jnp.mean(x * x, axis=-1, keepdims=True) + EPSILON) * gain
    quarter = CHANNEL_WIDTH // 4
    out = (
        y * cosine
        + pltpu.roll(y, CHANNEL_WIDTH - quarter, 1) * sine_a
        + pltpu.roll(y, quarter, 1) * sine_b
    )
    return out.astype(BF)


def dot(a, b):
    return jnp.dot(a, b, preferred_element_type=F32)


def layer_kernel(
    dims,
    skip_ref, q_ref, k_ref, v_ref, qg_ref, kg_ref, soft_ref, cos_ref, sa_ref, sb_ref,
    gain_ref, route_ref, ids_ref, wo_hbm, wg_hbm, wu_hbm, wd_hbm,
    out_ref,
    kk, vv, qs, sc, attn, pt, pk,
    p_send, p_recv, p_own, py_send, py_recv, mid,
    disp, xg, xn, r_send, r_recv, r_own, ry_send, ry_recv, ret, back,
    wo, wg, wu, wd,
    w_sem, k_s, k_r, v_s, v_r, pa_s, pa_r, py_s, py_r, d_s, d_r,
    gp_s, gp_r, gy_s, gy_r, gf_s, gf_r, rp_s, rp_r, ry_s, ry_r, b_s, b_r,
):
    n, m, tok, width, share, heads, lkv, capp, nch = dims
    A = m // CORES
    CW = CHANNEL_WIDTH
    me = lax.axis_index("sp")
    t = lax.axis_index("tp")
    a_pos = t // CORES
    core = t % CORES
    other = 1 - core
    partner = (me, a_pos * CORES + other)
    G = n // nch
    R = G * capp

    def sp_up(j):
        return (lax.rem(me + j, n), t)

    def sp_down(j):
        return (lax.rem(me + n - j, n), t)

    def a_at(i):
        return lax.rem(a_pos + i, A)

    def y_peer(i):
        return (me, a_at(i) * CORES + core)

    def cols_of(i, c):
        return pl.ds(pl.multiple_of((a_at(i) * CORES + c) * share, share), share)

    my_cols = pl.ds(pl.multiple_of(t * share, share), share)

    sends = []

    def remote(src, dst, ss, rs, dev):
        return pltpu.make_async_remote_copy(
            src_ref=src, dst_ref=dst, send_sem=ss, recv_sem=rs, device_id=dev, device_id_type=MESH
        )

    def go(cp):
        cp.start()
        sends.append(cp)
        return cp

    loads = [
        pltpu.make_async_copy(wo_hbm, wo, w_sem.at[0]),
        pltpu.make_async_copy(wg_hbm.at[0], wg, w_sem.at[1]),
        pltpu.make_async_copy(wu_hbm.at[0], wu, w_sem.at[2]),
        pltpu.make_async_copy(wd_hbm.at[0], wd, w_sem.at[3]),
    ]
    for cp in loads:
        cp.start()

    barrier = pltpu.get_barrier_semaphore()
    peers = [sp_up(j) for j in range(1, n)] + [partner] + [y_peer(i) for i in range(1, A)]
    for dev in peers:
        pl.semaphore_signal(barrier, inc=1, device_id=dev, device_id_type=MESH)

    first = (t * heads) // GROUP
    kv_cols = pl.ds(pl.multiple_of(first * CW, CW), lkv * CW)
    cosine, sine_a, sine_b = cos_ref[...], sa_ref[...], sb_ref[...]
    k_in = k_ref[:, kv_cols]
    for h in range(lkv):
        kk[0, :, h * CW:(h + 1) * CW] = norm_turn(
            k_in[:, h * CW:(h + 1) * CW], kg_ref[...], cosine, sine_a, sine_b
        )
    vv[0] = v_ref[:, kv_cols]
    pl.semaphore_wait(barrier, len(peers))
    k_cp, v_cp = {}, {}
    for j in range(1, n):
        k_cp[j] = go(remote(kk.at[0], kk.at[j], k_s.at[j], k_r.at[j], sp_up(j)))
    for j in range(1, n):
        v_cp[j] = go(remote(vv.at[0], vv.at[j], v_s.at[j], v_r.at[j], sp_up(j)))

    for h in range(heads):
        qs[h] = norm_turn(q_ref[:, h * CW:(h + 1) * CW], qg_ref[...], cosine, sine_a, sine_b)

    def column(row):
        return jnp.transpose(jnp.broadcast_to(row, (tok, tok)))[:, 0:1]

    rel = ids_ref[...] - me
    rel = jnp.where(rel < 0, rel + n, rel).astype(F32)
    rel = [column(rel[c:c + 1, :]) for c in range(2)]
    route = [column(route_ref[c:c + 1, :]) for c in range(2)]
    top = jnp.maximum(route[0], route[1])
    e0, e1 = jnp.exp(route[0] - top), jnp.exp(route[1] - top)
    weight = [e0 / (e0 + e1), e1 / (e0 + e1)]
    lanes = -(-n // 128) * 128
    lane_id = lax.broadcasted_iota(jnp.int32, (tok, lanes), 1).astype(F32)
    hot = [(rel[c] == lane_id).astype(F32) for c in range(2)]
    lower = (
        lax.broadcasted_iota(jnp.int32, (tok, tok), 1)
        < lax.broadcasted_iota(jnp.int32, (tok, tok), 0)
    ).astype(F32)
    rank = dot(lower.astype(BF), (hot[0] + hot[1]).astype(BF))
    slot_id = lax.broadcasted_iota(jnp.int32, (tok, n * capp), 1).astype(F32)
    picks = []
    for c in range(2):
        place = rel[c] * capp + jnp.sum(hot[c] * rank, axis=1, keepdims=True)
        picks.append((slot_id == place).astype(F32))
        pk[c] = picks[c].astype(BF)
    pt[...] = jnp.transpose(picks[0] + picks[1]).astype(BF)

    group = heads // lkv
    for j in range(n):
        if j:
            k_cp[j].wait_recv()
        for g in range(lkv):
            qg = qs[g * group:(g + 1) * group].reshape(group * tok, CW)
            s = lax.dot_general(
                qg, kk[j, :, g * CW:(g + 1) * CW], (((1,), (1,)), ((), ())),
                preferred_element_type=F32,
            )
            sc[pl.ds(g * group * tok, group * tok), j * tok:(j + 1) * tok] = s
    for j in range(1, n):
        v_cp[j].wait_recv()
    for h in range(heads):
        g = h // group
        s = sc[h * tok:(h + 1) * tok, :] * (soft_ref[h] * (1.0 / math.sqrt(CW)))
        e = jnp.exp(s - jnp.max(s, axis=-1, keepdims=True))
        total = jnp.sum(e, axis=-1, keepdims=True)
        v_all = vv[:, :, g * CW:(g + 1) * CW].reshape(n * tok, CW)
        attn[:, h * CW:(h + 1) * CW] = (dot(e.astype(BF), v_all) / total).astype(BF)

    loads[0].wait()
    att = attn[...]
    order = list(range(1, A)) + [0]
    pa_cp, py_cp = {}, {}
    for i in order:
        p_send[i] = dot(att, wo[:, cols_of(i, other)]).astype(BF)
        pa_cp[i] = go(remote(p_send.at[i], p_recv.at[i], pa_s.at[i], pa_r.at[i], partner))
    for i in order:
        p_own[i] = dot(att, wo[:, cols_of(i, core)])
    for i in range(1, A):
        pa_cp[i].wait_recv()
        py_send[i] = (p_own[i] + p_recv[i].astype(F32)).astype(BF)
        py_cp[i] = go(remote(py_send.at[i], py_recv.at[i], py_s.at[i], py_r.at[i], y_peer(i)))
    pa_cp[0].wait_recv()
    acc = p_own[0] + p_recv[0].astype(F32)
    for i in range(1, A):
        py_cp[i].wait_recv()
        acc = acc + py_recv[i].astype(F32)
    mid[...] = (skip_ref[:, my_cols].astype(F32) + acc.astype(BF).astype(F32)).astype(BF)

    disp[...] = dot(pt[...], mid[...]).astype(BF)
    d_cp = {}
    for j in range(1, n):
        d_cp[j] = go(remote(
            disp.at[pl.ds(j * capp, capp)], xg.at[pl.ds(j * capp, capp), my_cols],
            d_s.at[j], d_r.at[j], sp_up(j),
        ))
    xg[pl.ds(0, capp), my_cols] = disp[pl.ds(0, capp), :]

    gp_cp, gy_cp, gf_cp, rp_cp, ry_cp, b_cp = {}, {}, {}, {}, {}, {}

    def spread(ch):
        for j in range(ch * G, (ch + 1) * G):
            if j:
                d_cp[j].wait_recv()
        mine = xg.at[pl.ds(ch * R, R), my_cols]
        for i in range(1, A):
            gy_cp[ch, i] = go(remote(mine, mine, gy_s.at[ch, i], gy_r.at[ch, i], y_peer(i)))
        gp_cp[ch] = go(remote(mine, mine, gp_s.at[ch], gp_r.at[ch], partner))

    def forward(ch):
        for i in range(1, A):
            gy_cp[ch, i].wait_recv()
            piece = xg.at[pl.ds(ch * R, R), cols_of(A - i, core)]
            gf_cp[ch, i] = go(remote(piece, piece, gf_s.at[ch, i], gf_r.at[ch, i], partner))

    def serve(ch):
        rows = pl.ds(ch * R, R)
        gp_cp[ch].wait_recv()
        for i in range(1, A):
            gf_cp[ch, i].wait_recv()
        x = xg[rows, :].astype(F32)
        xn[...] = (
            x * lax.rsqrt(jnp.mean(x * x, axis=-1, keepdims=True) + EPSILON) * gain_ref[...]
        ).astype(BF)
        if ch == 0:
            loads[1].wait()
            loads[2].wait()
        x = xn[...]
        gate = dot(x, wg[...])
        up = dot(x, wu[...])
        hidden = (gate / (1.0 + jnp.exp(-gate)) * up).astype(BF)
        if ch == 0:
            loads[3].wait()
        for i in order:
            r_send[ch, i] = dot(hidden, wd[:, cols_of(i, other)]).astype(BF)
            rp_cp[ch, i] = go(remote(
                r_send.at[ch, i], r_recv.at[ch, i], rp_s.at[ch, i], rp_r.at[ch, i], partner
            ))
        for i in order:
            r_own[ch, i] = dot(hidden, wd[:, cols_of(i, core)])

    def join(ch):
        for i in range(1, A):
            rp_cp[ch, i].wait_recv()
            ry_send[ch, i] = (r_own[ch, i] + r_recv[ch, i].astype(F32)).astype(BF)
            ry_cp[ch, i] = go(remote(
                ry_send.at[ch, i], ry_recv.at[ch, i], ry_s.at[ch, i], ry_r.at[ch, i], y_peer(i)
            ))

    def give_back(ch):
        rp_cp[ch, 0].wait_recv()
        acc = r_own[ch, 0] + r_recv[ch, 0].astype(F32)
        for i in range(1, A):
            ry_cp[ch, i].wait_recv()
            acc = acc + ry_recv[ch, i].astype(F32)
        ret[pl.ds(ch * R, R), :] = acc.astype(BF)
        for j in range(ch * G, (ch + 1) * G):
            rows = pl.ds(j * capp, capp)
            if j:
                b_cp[j] = go(remote(ret.at[rows], back.at[rows], b_s.at[j], b_r.at[j], sp_down(j)))
            else:
                back[rows, :] = ret[rows, :]

    stages = (spread, forward, serve, join, give_back)
    for step in range(nch + len(stages) - 1):
        for late, stage in enumerate(stages):
            if 0 <= step - late < nch:
                stage(step - late)

    for j in range(1, n):
        b_cp[j].wait_recv()
    got = back[...]
    out = weight[0] * dot(pk[0], got) + weight[1] * dot(pk[1], got)
    out_ref[...] = (mid[...].astype(F32) + out).astype(BF)
    for cp in sends:
        cp.wait_send()


def shards(
    skip, q, k, v, q_gain, k_gain, soft, mix, gain, route, ids, w_gate, w_up, w_down
):
    n, m = lax.axis_size("sp"), lax.axis_size("tp")
    tok, width = skip.shape
    share = width // m
    heads = q.shape[1] // CHANNEL_WIDTH
    lkv = max(1, heads // GROUP)
    cap = max(2, 3 * tok * ids.shape[1] // (2 * n))
    capp = -(-cap // 16) * 16
    nch = math.gcd(n, 4)
    A = m // CORES
    eff = w_gate.shape[2]
    rows_all = n * capp
    R = rows_all // nch
    kvw = lkv * CHANNEL_WIDTH
    positions = lax.axis_index("sp") * tok + jnp.arange(tok, dtype=jnp.int32)
    cosine, sine_a, sine_b = turn_tables(positions)
    vm = pl.BlockSpec(memory_space=pltpu.VMEM)
    hbm = pl.BlockSpec(memory_space=pl.ANY)
    dma = pltpu.SemaphoreType.DMA
    dims = (n, m, tok, width, share, heads, lkv, capp, nch)
    pair = (nch, A)
    call = pl.pallas_call(
        functools.partial(layer_kernel, dims),
        out_shape=jax.ShapeDtypeStruct((tok, share), BF),
        in_specs=[vm] * 6 + [pl.BlockSpec(memory_space=pltpu.SMEM)] + [vm] * 6 + [hbm] * 4,
        out_specs=vm,
        scratch_shapes=[
            pltpu.VMEM((n, tok, kvw), BF),
            pltpu.VMEM((n, tok, kvw), BF),
            pltpu.VMEM((heads, tok, CHANNEL_WIDTH), BF),
            pltpu.VMEM((heads * tok, n * tok), F32),
            pltpu.VMEM((tok, heads * CHANNEL_WIDTH), BF),
            pltpu.VMEM((rows_all, tok), BF),
            pltpu.VMEM((2, tok, rows_all), BF),
            pltpu.VMEM((A, tok, share), BF),
            pltpu.VMEM((A, tok, share), BF),
            pltpu.VMEM((A, tok, share), F32),
            pltpu.VMEM((A, tok, share), BF),
            pltpu.VMEM((A, tok, share), BF),
            pltpu.VMEM((tok, share), BF),
            pltpu.VMEM((rows_all, share), BF),
            pltpu.VMEM((rows_all, width), BF),
            pltpu.VMEM((R, width), BF),
            pltpu.VMEM(pair + (R, share), BF),
            pltpu.VMEM(pair + (R, share), BF),
            pltpu.VMEM(pair + (R, share), F32),
            pltpu.VMEM(pair + (R, share), BF),
            pltpu.VMEM(pair + (R, share), BF),
            pltpu.VMEM((rows_all, share), BF),
            pltpu.VMEM((rows_all, share), BF),
            pltpu.VMEM(mix.shape, BF),
            pltpu.VMEM(w_gate.shape[1:], BF),
            pltpu.VMEM(w_up.shape[1:], BF),
            pltpu.VMEM(w_down.shape[1:], BF),
            dma((4,)),
            dma((n,)), dma((n,)), dma((n,)), dma((n,)),
            dma((A,)), dma((A,)), dma((A,)), dma((A,)),
            dma((n,)), dma((n,)),
            dma((nch,)), dma((nch,)), dma(pair), dma(pair), dma(pair), dma(pair),
            dma(pair), dma(pair), dma(pair), dma(pair),
            dma((n,)), dma((n,)),
        ],
        compiler_params=pltpu.CompilerParams(
            collective_id=0, has_side_effects=True, vmem_limit_bytes=56 * 1024 * 1024
        ),
    )
    return call(
        skip, q, k, v, q_gain.reshape(1, -1), k_gain.reshape(1, -1), soft,
        cosine, sine_a, sine_b, gain.reshape(1, -1), route.T, ids.T, mix, w_gate, w_up, w_down,
    )


def solution(mesh):
    in_specs = (
        P("sp", None),
        P("sp", "tp"),
        P("sp", None),
        P("sp", None),
        P(),
        P(),
        P("tp"),
        P("tp", None),
        P(),
        P("sp", None),
        P("sp", None),
        P("sp", None, "tp"),
        P("sp", None, "tp"),
        P("sp", "tp", None),
    )
    out_specs = P("sp", "tp")
    return jax.shard_map(shards, mesh=mesh, in_specs=in_specs, out_specs=out_specs, check_vma=False)
```

```python
import functools
import math

import jax
import jax.numpy as jnp
from jax import lax
from jax.experimental import pallas as pl
from jax.experimental.pallas import tpu as pltpu
from jax.sharding import PartitionSpec as P

CHANNEL_WIDTH = 128
GROUP = 4
GRID_W = 64
CORES = 2
EPSILON = 1e-06
MESH = pl.DeviceIdType.MESH
BF = jnp.bfloat16
F32 = jnp.float32


def turn_tables(positions):
    quarter = CHANNEL_WIDTH // 4
    frequency = 10000.0 ** (-jnp.arange(quarter, dtype=F32) / quarter)
    rows = (positions // GRID_W).astype(F32)[:, None] * frequency[None, :]
    cols = (positions % GRID_W).astype(F32)[:, None] * frequency[None, :]
    angles = jnp.concatenate([rows, rows, cols, cols], axis=1)
    cosine = jnp.cos(angles)
    sine = jnp.sin(angles)
    lane = jnp.arange(CHANNEL_WIDTH) // quarter
    first = (lane % 2 == 0)[None, :]
    return cosine, jnp.where(first, -sine, 0.0), jnp.where(first, 0.0, sine)


def norm_turn(x, gain, cosine, sine_a, sine_b):
    x = x.astype(F32)
    y = x * lax.rsqrt(jnp.mean(x * x, axis=-1, keepdims=True) + EPSILON) * gain
    quarter = CHANNEL_WIDTH // 4
    out = (
        y * cosine
        + pltpu.roll(y, CHANNEL_WIDTH - quarter, 1) * sine_a
        + pltpu.roll(y, quarter, 1) * sine_b
    )
    return out.astype(BF)


def dot(a, b):
    return jnp.dot(a, b, preferred_element_type=F32)


def layer_kernel(
    dims,
    skip_ref, q_ref, k_ref, v_ref, qg_ref, kg_ref, soft_ref, cos_ref, sa_ref, sb_ref,
    gain_ref, route_ref, ids_ref, wo_hbm, wg_hbm, wu_hbm, wd_hbm,
    out_ref,
    kk, vv, qs, sc, attn, pt, pk,
    p_send, p_recv, p_own, py_send, py_recv, mid,
    disp, xg, xn, r_send, r_recv, r_own, ry_send, ry_recv, ret, back,
    wo, wg, wu, wd,
    w_sem, k_s, k_r, v_s, v_r, pa_s, pa_r, py_s, py_r, d_s, d_r,
    gp_s, gp_r, gy_s, gy_r, gf_s, gf_r, rp_s, rp_r, ry_s, ry_r, b_s, b_r,
):
    n, m, tok, width, share, heads, lkv, capp, nch = dims
    A = m // CORES
    CW = CHANNEL_WIDTH
    me = lax.axis_index("sp")
    t = lax.axis_index("tp")
    a_pos = t // CORES
    core = t % CORES
    other = 1 - core
    partner = (me, a_pos * CORES + other)
    G = n // nch
    R = G * capp

    def sp_up(j):
        return (lax.rem(me + j, n), t)

    def sp_down(j):
        return (lax.rem(me + n - j, n), t)

    def a_at(i):
        return lax.rem(a_pos + i, A)

    def y_peer(i):
        return (me, a_at(i) * CORES + core)

    def cols_of(i, c):
        return pl.ds(pl.multiple_of((a_at(i) * CORES + c) * share, share), share)

    my_cols = pl.ds(pl.multiple_of(t * share, share), share)

    sends = []

    def remote(src, dst, ss, rs, dev):
        return pltpu.make_async_remote_copy(
            src_ref=src, dst_ref=dst, send_sem=ss, recv_sem=rs, device_id=dev, device_id_type=MESH
        )

    def go(cp):
        cp.start()
        sends.append(cp)
        return cp

    loads = [
        pltpu.make_async_copy(wo_hbm, wo, w_sem.at[0]),
        pltpu.make_async_copy(wg_hbm.at[0], wg, w_sem.at[1]),
        pltpu.make_async_copy(wu_hbm.at[0], wu, w_sem.at[2]),
        pltpu.make_async_copy(wd_hbm.at[0], wd, w_sem.at[3]),
    ]
    for cp in loads:
        cp.start()

    barrier = pltpu.get_barrier_semaphore()
    peers = [sp_up(j) for j in range(1, n)] + [partner] + [y_peer(i) for i in range(1, A)]
    for dev in peers:
        pl.semaphore_signal(barrier, inc=1, device_id=dev, device_id_type=MESH)

    first = (t * heads) // GROUP
    kv_cols = pl.ds(pl.multiple_of(first * CW, CW), lkv * CW)
    cosine, sine_a, sine_b = cos_ref[...], sa_ref[...], sb_ref[...]
    k_in = k_ref[:, kv_cols]
    for h in range(lkv):
        kk[0, :, h * CW:(h + 1) * CW] = norm_turn(
            k_in[:, h * CW:(h + 1) * CW], kg_ref[...], cosine, sine_a, sine_b
        )
    vv[0] = v_ref[:, kv_cols]
    pl.semaphore_wait(barrier, len(peers))
    X = math.gcd(n, 2)
    beside = (me + 1 - 2 * lax.rem(me, 2), t)
    k_cp, v_cp = {}, {}

    def to_below(cps, buf, ss, rs):
        for j in range(X, n, X):
            cps[j] = go(remote(buf.at[0], buf.at[j], ss.at[j], rs.at[j], sp_up(j)))

    def to_side(cps, buf, ss, rs, j):
        if X > 1:
            cps[j + 1] = go(remote(buf.at[j], buf.at[j + 1], ss.at[j + 1], rs.at[j + 1], beside))

    to_below(k_cp, kk, k_s, k_r)
    to_side(k_cp, kk, k_s, k_r, 0)
    to_below(v_cp, vv, v_s, v_r)
    to_side(v_cp, vv, v_s, v_r, 0)

    for h in range(heads):
        qs[h] = norm_turn(q_ref[:, h * CW:(h + 1) * CW], qg_ref[...], cosine, sine_a, sine_b)

    def column(row):
        return jnp.transpose(jnp.broadcast_to(row, (tok, tok)))[:, 0:1]

    rel = ids_ref[...] - me
    rel = jnp.where(rel < 0, rel + n, rel).astype(F32)
    rel = [column(rel[c:c + 1, :]) for c in range(2)]
    route = [column(route_ref[c:c + 1, :]) for c in range(2)]
    top = jnp.maximum(route[0], route[1])
    e0, e1 = jnp.exp(route[0] - top), jnp.exp(route[1] - top)
    weight = [e0 / (e0 + e1), e1 / (e0 + e1)]
    lanes = -(-n // 128) * 128
    lane_id = lax.broadcasted_iota(jnp.int32, (tok, lanes), 1).astype(F32)
    hot = [(rel[c] == lane_id).astype(F32) for c in range(2)]
    lower = (
        lax.broadcasted_iota(jnp.int32, (tok, tok), 1)
        < lax.broadcasted_iota(jnp.int32, (tok, tok), 0)
    ).astype(F32)
    rank = dot(lower.astype(BF), (hot[0] + hot[1]).astype(BF))
    slot_id = lax.broadcasted_iota(jnp.int32, (tok, n * capp), 1).astype(F32)
    picks = []
    for c in range(2):
        place = rel[c] * capp + jnp.sum(hot[c] * rank, axis=1, keepdims=True)
        picks.append((slot_id == place).astype(F32))
        pk[c] = picks[c].astype(BF)
    pt[...] = jnp.transpose(picks[0] + picks[1]).astype(BF)

    group = heads // lkv

    def score(j):
        for g in range(lkv):
            qg = qs[g * group:(g + 1) * group].reshape(group * tok, CW)
            s = lax.dot_general(
                qg, kk[j, :, g * CW:(g + 1) * CW], (((1,), (1,)), ((), ())),
                preferred_element_type=F32,
            )
            sc[pl.ds(g * group * tok, group * tok), j * tok:(j + 1) * tok] = s

    for j in range(X, n, X):
        k_cp[j].wait_recv()
        to_side(k_cp, kk, k_s, k_r, j)
        if j == X:
            score(0)
        score(j)
    for j in range(X, n, X):
        v_cp[j].wait_recv()
        to_side(v_cp, vv, v_s, v_r, j)
    for j in range(0, n, X):
        for side in range(1, X):
            k_cp[j + side].wait_recv()
            score(j + side)
    for j in range(0, n, X):
        for side in range(1, X):
            v_cp[j + side].wait_recv()
    for h in range(heads):
        g = h // group
        s = sc[h * tok:(h + 1) * tok, :] * (soft_ref[h] * (1.0 / math.sqrt(CW)))
        e = jnp.exp(s - jnp.max(s, axis=-1, keepdims=True))
        total = jnp.sum(e, axis=-1, keepdims=True)
        v_all = vv[:, :, g * CW:(g + 1) * CW].reshape(n * tok, CW)
        attn[:, h * CW:(h + 1) * CW] = (dot(e.astype(BF), v_all) / total).astype(BF)

    loads[0].wait()
    att = attn[...]
    order = list(range(1, A)) + [0]
    pa_cp, py_cp = {}, {}
    for i in order:
        p_send[i] = dot(att, wo[:, cols_of(i, other)]).astype(BF)
        pa_cp[i] = go(remote(p_send.at[i], p_recv.at[i], pa_s.at[i], pa_r.at[i], partner))
    for i in order:
        p_own[i] = dot(att, wo[:, cols_of(i, core)])
    for i in range(1, A):
        pa_cp[i].wait_recv()
        py_send[i] = (p_own[i] + p_recv[i].astype(F32)).astype(BF)
        py_cp[i] = go(remote(py_send.at[i], py_recv.at[i], py_s.at[i], py_r.at[i], y_peer(i)))
    pa_cp[0].wait_recv()
    acc = p_own[0] + p_recv[0].astype(F32)
    for i in range(1, A):
        py_cp[i].wait_recv()
        acc = acc + py_recv[i].astype(F32)
    mid[...] = (skip_ref[:, my_cols].astype(F32) + acc.astype(BF).astype(F32)).astype(BF)

    disp[...] = dot(pt[...], mid[...]).astype(BF)
    d_cp = {}
    for j in range(1, n):
        d_cp[j] = go(remote(
            disp.at[pl.ds(j * capp, capp)], xg.at[pl.ds(j * capp, capp), my_cols],
            d_s.at[j], d_r.at[j], sp_up(j),
        ))
    xg[pl.ds(0, capp), my_cols] = disp[pl.ds(0, capp), :]

    gp_cp, gy_cp, gf_cp, rp_cp, ry_cp, b_cp = {}, {}, {}, {}, {}, {}

    def spread(ch):
        for j in range(ch * G, (ch + 1) * G):
            if j:
                d_cp[j].wait_recv()
        mine = xg.at[pl.ds(ch * R, R), my_cols]
        for i in range(1, A):
            gy_cp[ch, i] = go(remote(mine, mine, gy_s.at[ch, i], gy_r.at[ch, i], y_peer(i)))
        gp_cp[ch] = go(remote(mine, mine, gp_s.at[ch], gp_r.at[ch], partner))

    def forward(ch):
        for i in range(1, A):
            gy_cp[ch, i].wait_recv()
            piece = xg.at[pl.ds(ch * R, R), cols_of(A - i, core)]
            gf_cp[ch, i] = go(remote(piece, piece, gf_s.at[ch, i], gf_r.at[ch, i], partner))

    def serve(ch):
        rows = pl.ds(ch * R, R)
        gp_cp[ch].wait_recv()
        for i in range(1, A):
            gf_cp[ch, i].wait_recv()
        x = xg[rows, :].astype(F32)
        xn[...] = (
            x * lax.rsqrt(jnp.mean(x * x, axis=-1, keepdims=True) + EPSILON) * gain_ref[...]
        ).astype(BF)
        if ch == 0:
            loads[1].wait()
            loads[2].wait()
        x = xn[...]
        gate = dot(x, wg[...])
        up = dot(x, wu[...])
        hidden = (gate / (1.0 + jnp.exp(-gate)) * up).astype(BF)
        if ch == 0:
            loads[3].wait()
        for i in order:
            r_send[ch, i] = dot(hidden, wd[:, cols_of(i, other)]).astype(BF)
            rp_cp[ch, i] = go(remote(
                r_send.at[ch, i], r_recv.at[ch, i], rp_s.at[ch, i], rp_r.at[ch, i], partner
            ))
        for i in order:
            r_own[ch, i] = dot(hidden, wd[:, cols_of(i, core)])

    def join(ch):
        for i in range(1, A):
            rp_cp[ch, i].wait_recv()
            ry_send[ch, i] = (r_own[ch, i] + r_recv[ch, i].astype(F32)).astype(BF)
            ry_cp[ch, i] = go(remote(
                ry_send.at[ch, i], ry_recv.at[ch, i], ry_s.at[ch, i], ry_r.at[ch, i], y_peer(i)
            ))

    def give_back(ch):
        rp_cp[ch, 0].wait_recv()
        acc = r_own[ch, 0] + r_recv[ch, 0].astype(F32)
        for i in range(1, A):
            ry_cp[ch, i].wait_recv()
            acc = acc + ry_recv[ch, i].astype(F32)
        ret[pl.ds(ch * R, R), :] = acc.astype(BF)
        for j in range(ch * G, (ch + 1) * G):
            rows = pl.ds(j * capp, capp)
            if j:
                b_cp[j] = go(remote(ret.at[rows], back.at[rows], b_s.at[j], b_r.at[j], sp_down(j)))
            else:
                back[rows, :] = ret[rows, :]

    stages = (spread, forward, serve, join, give_back)
    for step in range(nch + len(stages) - 1):
        for late, stage in enumerate(stages):
            if 0 <= step - late < nch:
                stage(step - late)

    for j in range(1, n):
        b_cp[j].wait_recv()
    got = back[...]
    out = weight[0] * dot(pk[0], got) + weight[1] * dot(pk[1], got)
    out_ref[...] = (mid[...].astype(F32) + out).astype(BF)
    for cp in sends:
        cp.wait_send()


def shards(
    skip, q, k, v, q_gain, k_gain, soft, mix, gain, route, ids, w_gate, w_up, w_down
):
    n, m = lax.axis_size("sp"), lax.axis_size("tp")
    tok, width = skip.shape
    share = width // m
    heads = q.shape[1] // CHANNEL_WIDTH
    lkv = max(1, heads // GROUP)
    cap = max(2, 3 * tok * ids.shape[1] // (2 * n))
    capp = -(-cap // 16) * 16
    nch = math.gcd(n, 4)
    A = m // CORES
    eff = w_gate.shape[2]
    rows_all = n * capp
    R = rows_all // nch
    kvw = lkv * CHANNEL_WIDTH
    positions = lax.axis_index("sp") * tok + jnp.arange(tok, dtype=jnp.int32)
    cosine, sine_a, sine_b = turn_tables(positions)
    vm = pl.BlockSpec(memory_space=pltpu.VMEM)
    hbm = pl.BlockSpec(memory_space=pl.ANY)
    dma = pltpu.SemaphoreType.DMA
    dims = (n, m, tok, width, share, heads, lkv, capp, nch)
    pair = (nch, A)
    call = pl.pallas_call(
        functools.partial(layer_kernel, dims),
        out_shape=jax.ShapeDtypeStruct((tok, share), BF),
        in_specs=[vm] * 6 + [pl.BlockSpec(memory_space=pltpu.SMEM)] + [vm] * 6 + [hbm] * 4,
        out_specs=vm,
        scratch_shapes=[
            pltpu.VMEM((n, tok, kvw), BF),
            pltpu.VMEM((n, tok, kvw), BF),
            pltpu.VMEM((heads, tok, CHANNEL_WIDTH), BF),
            pltpu.VMEM((heads * tok, n * tok), F32),
            pltpu.VMEM((tok, heads * CHANNEL_WIDTH), BF),
            pltpu.VMEM((rows_all, tok), BF),
            pltpu.VMEM((2, tok, rows_all), BF),
            pltpu.VMEM((A, tok, share), BF),
            pltpu.VMEM((A, tok, share), BF),
            pltpu.VMEM((A, tok, share), F32),
            pltpu.VMEM((A, tok, share), BF),
            pltpu.VMEM((A, tok, share), BF),
            pltpu.VMEM((tok, share), BF),
            pltpu.VMEM((rows_all, share), BF),
            pltpu.VMEM((rows_all, width), BF),
            pltpu.VMEM((R, width), BF),
            pltpu.VMEM(pair + (R, share), BF),
            pltpu.VMEM(pair + (R, share), BF),
            pltpu.VMEM(pair + (R, share), F32),
            pltpu.VMEM(pair + (R, share), BF),
            pltpu.VMEM(pair + (R, share), BF),
            pltpu.VMEM((rows_all, share), BF),
            pltpu.VMEM((rows_all, share), BF),
            pltpu.VMEM(mix.shape, BF),
            pltpu.VMEM(w_gate.shape[1:], BF),
            pltpu.VMEM(w_up.shape[1:], BF),
            pltpu.VMEM(w_down.shape[1:], BF),
            dma((4,)),
            dma((n,)), dma((n,)), dma((n,)), dma((n,)),
            dma((A,)), dma((A,)), dma((A,)), dma((A,)),
            dma((n,)), dma((n,)),
            dma((nch,)), dma((nch,)), dma(pair), dma(pair), dma(pair), dma(pair),
            dma(pair), dma(pair), dma(pair), dma(pair),
            dma((n,)), dma((n,)),
        ],
        compiler_params=pltpu.CompilerParams(
            collective_id=0, has_side_effects=True, vmem_limit_bytes=56 * 1024 * 1024
        ),
    )
    return call(
        skip, q, k, v, q_gain.reshape(1, -1), k_gain.reshape(1, -1), soft,
        cosine, sine_a, sine_b, gain.reshape(1, -1), route.T, ids.T, mix, w_gate, w_up, w_down,
    )


def solution(mesh):
    in_specs = (
        P("sp", None),
        P("sp", "tp"),
        P("sp", None),
        P("sp", None),
        P(),
        P(),
        P("tp"),
        P("tp", None),
        P(),
        P("sp", None),
        P("sp", None),
        P("sp", None, "tp"),
        P("sp", None, "tp"),
        P("sp", "tp", None),
    )
    out_specs = P("sp", "tp")
    return jax.shard_map(shards, mesh=mesh, in_specs=in_specs, out_specs=out_specs, check_vma=False)
```
